512 devices in a mesh: ep: 32 (over z, core), tp: 16 (over y, x).
Axes of the slice: x: 4, y: 4, z: 16, core: 2. Of those that a mesh axis runs over, the one named last changes fastest.
Arguments:
- first_batch_queries: bfloat16 [8192, 1024], P('ep', 'tp'), may hold values from -6 to 6
- first_batch_keys: bfloat16 [8192, 1024], P('ep', 'tp'), may hold values from -6 to 6
- first_batch_values: bfloat16 [8192, 2048], P('ep', 'tp'), may hold values from -6 to 6
- output_gate_preactivation: bfloat16 [8192, 2048], P('ep', 'tp'), may hold values from -6 to 6
- decay_preactivation: bfloat16 [8192, 1024], P('ep', 'tp'), may hold values from -6 to 6
- channel_decay_bias: float32 [1024], P('tp')
- added_log_decay: float32 [16, 8192], P('tp', 'ep'), may hold values from -0.7 to 0
- head_norm_gain: float32 [2048], P('tp'), may hold values from 0.1 to 1.9
- attention_output_weight: bfloat16 [2048, 2048], P(None, 'tp'), may hold values from -0.125 to 0.125
- second_batch_rows: bfloat16 [3072, 2048], P('ep'), may hold values from -6 to 6
- expert_norm_gain: float32 [2048], replicated, may hold values from 0.1 to 1.9
- routed_expert_index: int32 [3072, 4], P('ep'), may hold values from 0 to 31, all different within a row; in each aligned block of 96 rows (0 to 95, 96 to 191, ...) at most 18 rows name the same one
- router_chosen_scores: float32 [3072, 4], P('ep'), may hold values from 0.1 to 1
- expert_gate_weight: bfloat16 [32, 2048, 4096], P('ep', None, 'tp'), may hold values from -0.125 to 0.125
- expert_up_weight: bfloat16 [32, 2048, 4096], P('ep', None, 'tp'), may hold values from -0.125 to 0.125
- expert_down_weight: bfloat16 [32, 4096, 2048], P('ep', None, 'tp'), may hold values from -0.09375 to 0.09375
- shared_gate_weight: bfloat16 [2048, 1024], P(None, 'tp'), may hold values from -0.125 to 0.125
- shared_up_weight: bfloat16 [2048, 1024], P(None, 'tp'), may hold values from -0.125 to 0.125
- shared_down_weight: bfloat16 [1024, 2048], P(None, 'tp'), may hold values from -0.1875 to 0.1875
Outputs:
- token_mixed: bfloat16 [8192, 2048], P('ep', 'tp')
- channel_mixed: bfloat16 [3072, 2048], P('ep', 'tp')
The draws below stay inside these ranges and needn't reach their ends.
Inputs may be any that keep to these rules, and one draw needn't show every extreme that they name: `routed_expert_index`: in each aligned block of 96 rows (the rows of one index of ep) no expert is named by more than 18 rows, a bound that some block reaches; a row names 4 different experts.
All inputs are finite; a program needn't handle non-finite values.
Results may differ from the reference program's by a relative error of at most 0.018.
Values may be sent and summed in bfloat16 or wider, within the bound.
A program may use at most 64 MiB of HBM per device.

```python
import math
from functools import partial
import jax
import jax.numpy as jnp
import numpy as np
from jax import lax

D = 2048
ATTENTION_HEADS = 16
DK = 64
DV = 128
BLOCK = 64
FFE = 4096
FFS = 1024
TOPK = 4
TOK_A = 256
TOK_B = 96
FIRST_TOKENS = 8192
TOKENS_B = 3072
EXPERTS = 32
CAP = 18


def draw_channel_decay_bias(key, part):
    key_kind, key_slow, key_fast = jax.random.split(jax.random.fold_in(key, 11), 3)
    share = 0.5
    slow_head = jax.random.uniform(key_kind, (ATTENTION_HEADS, 1), jnp.float32) < share
    slow_level = math.log(0.34 * FIRST_TOKENS) + jax.random.uniform(key_slow, (ATTENTION_HEADS, DK), jnp.float32, -0.5, 0.5)
    fast_level = jax.random.uniform(key_fast, (ATTENTION_HEADS, DK), jnp.float32, -1.0, 1.5)
    return jnp.where(slow_head, slow_level, fast_level).reshape(ATTENTION_HEADS * DK).astype(jnp.float32)


def draw_added_log_decay(key, part):
    key_rate, key_locations, key_dimension = jax.random.split(jax.random.fold_in(key, 23), 3)
    devices = FIRST_TOKENS // TOK_A
    device_rates = jnp.exp(jax.random.uniform(key_rate, (devices,), jnp.float32, math.log(0.1), math.log(1.0))) / FIRST_TOKENS
    baseline_log_decay = -jnp.repeat(device_rates, TOK_A)
    position_index = jnp.arange(FIRST_TOKENS, dtype=jnp.int32)
    half_length = FIRST_TOKENS // 2
    halves_start = jnp.array([0, half_length], dtype=jnp.int32)
    spike_positions = jax.random.randint(key_locations, (ATTENTION_HEADS, 2), 0, half_length) + halves_start[None, :]
    spike_magnitude = jnp.log(jax.random.uniform(key_dimension, (ATTENTION_HEADS, 2), jnp.float32, 0.5, 0.8))
    decay_spikes = jnp.sum(jnp.where(position_index[None, None, :] == spike_positions[:, :, None], spike_magnitude[:, :, None], 0.0), axis=1)
    return (baseline_log_decay[None, :] + decay_spikes).astype(jnp.float32)


def block_scale(rng, shape, cuts, low, top_value):
    gain, own = 1.0, jax.random.fold_in(rng, 6)
    for dim, parts in cuts:
        steps = jnp.exp(jax.random.uniform(jax.random.fold_in(own, dim), (parts,), jnp.float32, low / len(cuts), top_value / len(cuts)))
        gain = gain * jnp.repeat(steps, shape[dim] // parts).reshape([-1 if axis == dim else 1 for axis in range(len(shape))])
    return gain


def shared_out(key, own, number, rows, amount, top, bound, slope):
    sequence = jax.random.permutation(key, amount)
    heavy_load, ordinary = load_shares(amount, rows * top, bound, slope, True), load_shares(amount, rows * top, bound, slope, False)
    places = jnp.arange(amount)

    def named(lengths, rotation):
        used = int((lengths > 0).sum())
        fixed = max(1, used // 4)
        shifted = fixed + (places - fixed + rotation * (used - fixed)) % max(1, amount - fixed)
        return jnp.zeros((amount,), jnp.int32).at[sequence[jnp.where(places < fixed, places, shifted)]].set(jnp.asarray(lengths, jnp.int32))

    lengths = jnp.where(number % 4 == 0, named(heavy_load, number // 4), named(ordinary, number - number // 4 - 1))
    mixed = jax.random.permutation(jax.random.fold_in(own, 3), amount)
    source_of, receiver = mixed[0:amount // 2 * 2:2], mixed[1:amount // 2 * 2:2]
    room = jnp.minimum(lengths[source_of] - 1, bound - lengths[receiver]) // 2
    room = jnp.where((source_of == sequence[0]) | (receiver == sequence[0]) | (lengths[receiver] == 0), 0, jnp.maximum(room, 0))
    shifted = jax.random.randint(jax.random.fold_in(own, 4), (amount // 2,), 0, 1 << 20) % (room + 1)
    lengths = lengths.at[source_of].add(-shifted).at[receiver].add(shifted)
    labels = jnp.searchsorted(jnp.cumsum(lengths), jnp.arange(rows * top), side="right").astype(jnp.int32)
    table = labels.reshape(top, rows).T
    table = table[jax.random.permutation(jax.random.fold_in(own, 1), rows)]
    rotation = jax.random.randint(jax.random.fold_in(own, 2), (rows, 1), 0, top)
    return jnp.take_along_axis(table, (jnp.arange(top)[None, :] + rotation) % top, axis=1)


def load_shares(count, total, reach, skew, full):
    weights = [(1 << 20) // math.isqrt(grade ** skew) + 1 for grade in range(1, count + 1)]
    largest = reach if full else min(reach, max(-(-total // count), total * weights[0] // sum(weights)))
    least = 1 if total - largest >= count - 1 else 0
    counts, surplus = [largest] + [least] * (count - 1), total - largest - least * (count - 1)
    while surplus > 0:
        candidates = [i for i in range(1, count) if counts[i] < largest] or [i for i in range(1, count) if counts[i] < reach]
        whole, budget = sum([weights[i] for i in candidates]), surplus
        for i in candidates:
            extra = min(reach - counts[i], max(1, budget * weights[i] // whole), surplus)
            counts[i] = counts[i] + extra
            surplus = surplus - extra
    return np.array(counts)


def normal_values(key, dims, deviation, limit, pieces=(), kind=jnp.bfloat16):
    values = deviation * jax.random.normal(key, dims, jnp.float32)
    if pieces:
        values = values * block_scale(key, dims, pieces, -0.22, 0.18)
    return jnp.clip(values, -limit, limit).astype(kind)


def setup_inputs(seed: int = 0) -> dict:
    streams_of = jax.random.split(jax.random.key(seed), 20)
    first_batch_queries = normal_values(streams_of[0], (FIRST_TOKENS, ATTENTION_HEADS * DK), 1.0, 6.0, ((0, 32), (1, 16)))
    first_batch_keys = normal_values(streams_of[1], (FIRST_TOKENS, ATTENTION_HEADS * DK), 1.0, 6.0, ((0, 32), (1, 16)))
    first_batch_values = normal_values(streams_of[2], (FIRST_TOKENS, ATTENTION_HEADS * DV), 1.0, 6.0, ((0, 32), (1, 16)))
    output_gate_preactivation = normal_values(streams_of[3], (FIRST_TOKENS, ATTENTION_HEADS * DV), 1.0, 6.0, ((0, 32), (1, 16)))
    decay_preactivation = normal_values(streams_of[4], (FIRST_TOKENS, ATTENTION_HEADS * DK), 1.0, 6.0, ((0, 32), (1, 16)))
    channel_decay_bias = draw_channel_decay_bias(jax.random.fold_in(streams_of[19], 71), 0)
    added_log_decay = draw_added_log_decay(jax.random.fold_in(streams_of[19], 71), 0)
    head_norm_gain = jnp.clip(1.0 + 0.18 * jax.random.normal(streams_of[7], (ATTENTION_HEADS * DV,), jnp.float32), 0.1, 1.9)
    attention_output_weight = normal_values(streams_of[8], (ATTENTION_HEADS * DV, D), (ATTENTION_HEADS * DV) ** -0.5, 0.125, ((1, 16),))
    second_batch_rows = normal_values(streams_of[9], (TOKENS_B, D), 1.0, 6.0, ((0, 32),))
    expert_norm_gain = jnp.clip(1.0 + 0.18 * jax.random.normal(streams_of[10], (D,), jnp.float32), 0.1, 1.9)
    routed_expert_index_keys = jax.random.split(jax.random.fold_in(streams_of[11], 1), TOKENS_B // TOK_B)
    routed_expert_index_turns = jax.random.permutation(jax.random.fold_in(streams_of[11], 3), TOKENS_B // TOK_B)
    routed_expert_index = jax.vmap(lambda own, number: shared_out(jax.random.fold_in(streams_of[11], 2), own, number, TOK_B, EXPERTS, TOPK, CAP, 1))(routed_expert_index_keys, routed_expert_index_turns).reshape((TOKENS_B, TOPK))
    router_chosen_scores = jnp.clip(jnp.exp(math.log(1.0) - 2.3025851 * jax.random.uniform(streams_of[12], (TOKENS_B, TOPK), jnp.float32) ** block_scale(streams_of[12], (TOKENS_B, TOPK), ((0, 32),), -0.2, 0.2)), 0.1, 1.0)
    expert_gate_weight = normal_values(streams_of[13], (EXPERTS, D, FFE), D ** -0.5, 0.125, ((0, 32), (2, 16)))
    expert_up_weight = normal_values(streams_of[14], (EXPERTS, D, FFE), D ** -0.5, 0.125, ((0, 32), (2, 16)))
    expert_down_weight = normal_values(streams_of[15], (EXPERTS, FFE, D), FFE ** -0.5, 0.09375, ((0, 32), (2, 16)))
    shared_gate_weight = normal_values(streams_of[16], (D, FFS), D ** -0.5, 0.125, ((1, 16),))
    shared_up_weight = normal_values(streams_of[17], (D, FFS), D ** -0.5, 0.125, ((1, 16),))
    shared_down_weight = normal_values(streams_of[18], (FFS, D), FFS ** -0.5, 0.1875, ((1, 16),))
    return {"first_batch_queries": first_batch_queries, "first_batch_keys": first_batch_keys, "first_batch_values": first_batch_values, "output_gate_preactivation": output_gate_preactivation, "decay_preactivation": decay_preactivation, "channel_decay_bias": channel_decay_bias, "added_log_decay": added_log_decay, "head_norm_gain": head_norm_gain, "attention_output_weight": attention_output_weight, "second_batch_rows": second_batch_rows, "expert_norm_gain": expert_norm_gain, "routed_expert_index": routed_expert_index, "router_chosen_scores": router_chosen_scores, "expert_gate_weight": expert_gate_weight, "expert_up_weight": expert_up_weight, "expert_down_weight": expert_down_weight, "shared_gate_weight": shared_gate_weight, "shared_up_weight": shared_up_weight, "shared_down_weight": shared_down_weight}


epsilon = 1e-06
temper = 16.0
routed_scale = 2.5
largest_value = lax.Precision.HIGHEST

def head_norm(tensor, gain_rows):
    mean_square = lax.optimization_barrier(jnp.mean(tensor * tensor, axis=-1, keepdims=True))
    return tensor * lax.rsqrt(mean_square + epsilon) * gain_rows

def log_decay_values(decay_preactivation, channel_decay_bias, added_log_decay):
    number_of_heads = added_log_decay.shape[0]
    row_count = decay_preactivation.shape[0]
    logits = decay_preactivation.astype(jnp.float32) + channel_decay_bias[None, :]
    baseline_log_decay = (jax.nn.log_sigmoid(logits) / temper).reshape(row_count, number_of_heads, -1)
    return baseline_log_decay + jnp.transpose(added_log_decay)[:, :, None]

def gated_linear(queries, keys_all, values, decay_factors):
    row_count, number_of_heads, key_channel_width = queries.shape
    value_width = values.shape[-1]
    block_count = row_count // BLOCK

    def split_into_blocks(tensor):
        return tensor.reshape(block_count, BLOCK, number_of_heads, tensor.shape[-1]).transpose(0, 2, 1, 3)
    lower_mask = jnp.tril(jnp.ones((BLOCK, BLOCK), bool))

    def advance(carry_state, inputs):
        query_block, block_of_keys, block_of_values, decay_block = inputs
        running_state = jnp.cumsum(decay_block, axis=1)
        query_decayed = query_block * jnp.exp(running_state)
        key_raised = block_of_keys * jnp.exp(-running_state)
        attention_scores = jnp.einsum('hqd,hkd->hqk', query_decayed, key_raised, precision=largest_value)
        attention_scores = jnp.where(lower_mask, attention_scores, 0.0)
        within_block = jnp.einsum('gnx,gxy->gny', attention_scores, block_of_values, precision=largest_value)
        carried = jnp.einsum('hqd,hdv->hqv', query_decayed, carry_state, precision=largest_value)
        block_number_total = running_state[:, -1:, :]
        state_update = jnp.einsum('ien,ieg->ing', block_of_keys * jnp.exp(block_number_total - running_state), block_of_values, precision=largest_value)
        new_state = jnp.exp(block_number_total[:, 0, :])[..., None] * carry_state + state_update
        return (new_state, within_block + carried)
    start_state = jnp.zeros((number_of_heads, key_channel_width, value_width), jnp.float32)
    _, outputs = lax.scan(advance, start_state, (split_into_blocks(queries), split_into_blocks(keys_all), split_into_blocks(values), split_into_blocks(decay_factors)))
    return outputs.transpose(0, 2, 1, 3).reshape(row_count, number_of_heads, value_width)

def expert_slots(route_rows, experts, capacity):
    flat_ids = route_rows.reshape(-1)
    targets = jnp.arange(experts, dtype=jnp.int32)
    onehot = (flat_ids[:, None] == targets[None, :]).astype(jnp.int32)
    earlier = jnp.cumsum(onehot, axis=0) - onehot
    return (flat_ids * capacity + lax.optimization_barrier(jnp.sum(earlier * onehot, axis=1))).astype(jnp.int32)

def slot_owner(slot_ids, slot_count, top_count):
    matches = slot_ids[None, :] == jnp.arange(slot_count, dtype=jnp.int32)[:, None]
    token_ids = jnp.arange(slot_ids.shape[0], dtype=jnp.int32) // top_count
    return (lax.optimization_barrier(jnp.sum(jnp.where(matches, token_ids[None, :] + 1, 0), axis=1)) - 1).astype(jnp.int32)

def reference(first_batch_queries, first_batch_keys, first_batch_values, output_gate_preactivation, decay_preactivation, channel_decay_bias, added_log_decay, head_norm_gain, attention_output_weight, second_batch_rows, expert_norm_gain, routed_expert_index, router_chosen_scores, expert_gate_weight, expert_up_weight, expert_down_weight, shared_gate_weight, shared_up_weight, shared_down_weight):
    decay_factors = log_decay_values(decay_preactivation, channel_decay_bias, added_log_decay)
    queries = first_batch_queries.astype(jnp.float32).reshape(FIRST_TOKENS, ATTENTION_HEADS, DK)
    keys_all = first_batch_keys.astype(jnp.float32).reshape(FIRST_TOKENS, ATTENTION_HEADS, DK)
    values = first_batch_values.astype(jnp.float32).reshape(FIRST_TOKENS, ATTENTION_HEADS, DV)
    head_values = gated_linear(queries, keys_all, values, decay_factors)
    gate_rows = jax.nn.silu(output_gate_preactivation.astype(jnp.float32)).reshape(FIRST_TOKENS, ATTENTION_HEADS, DV)
    mixed_heads = head_norm(head_values, head_norm_gain.reshape(ATTENTION_HEADS, DV)) * gate_rows
    mixed_heads = mixed_heads.reshape(FIRST_TOKENS, ATTENTION_HEADS * DV).astype(jnp.bfloat16)
    token_mixed = jnp.dot(mixed_heads, attention_output_weight, preferred_element_type=jnp.float32).astype(jnp.bfloat16)
    features = second_batch_rows.astype(jnp.float32)
    normed = features * lax.rsqrt(lax.optimization_barrier(jnp.mean(features * features, axis=1, keepdims=True)) + epsilon)
    normed = (normed * expert_norm_gain[None, :]).astype(jnp.bfloat16)
    sources = TOKENS_B // TOK_B
    slot_count = EXPERTS * CAP
    block_routes = routed_expert_index.reshape(sources, TOK_B, TOPK)
    slot_ids = jax.vmap(partial(expert_slots, experts=EXPERTS, capacity=CAP))(block_routes)
    owners = jax.vmap(partial(slot_owner, slot_count=slot_count, top_count=TOPK))(slot_ids)
    offsets = (jnp.arange(sources, dtype=jnp.int32) * TOK_B)[:, None]
    global_owner = jnp.where(owners >= 0, owners + offsets, -1)
    per_expert = global_owner.reshape(sources, EXPERTS, CAP).transpose(1, 0, 2).reshape(EXPERTS, sources * CAP)

    def run_expert(inputs):
        owner_rows, gate_weight, up_weight, down_weight = inputs
        picked_rows = jnp.take(normed, jnp.maximum(owner_rows, 0), axis=0)
        rows_in = jnp.where((owner_rows >= 0)[:, None], picked_rows, jnp.zeros((), jnp.bfloat16))
        gate_value = jnp.dot(rows_in, gate_weight, preferred_element_type=jnp.float32)
        up_value = jnp.dot(rows_in, up_weight, preferred_element_type=jnp.float32)
        hidden = (jax.nn.silu(gate_value) * up_value).astype(jnp.bfloat16)
        return jnp.dot(hidden, down_weight, preferred_element_type=jnp.float32).astype(jnp.bfloat16)
    results = lax.map(run_expert, (per_expert, expert_gate_weight, expert_up_weight, expert_down_weight))
    expert_ids = block_routes.reshape(sources, -1)
    source_ids = jnp.arange(sources, dtype=jnp.int32)[:, None]
    flat_index = expert_ids * (sources * CAP) + source_ids * CAP + (slot_ids - expert_ids * CAP)
    picked = jnp.take(results.reshape(-1, D), flat_index.reshape(-1).astype(jnp.int32), axis=0)
    picked = picked.astype(jnp.float32).reshape(TOKENS_B, TOPK, D)
    weights = routed_scale * router_chosen_scores / lax.optimization_barrier(jnp.sum(router_chosen_scores, axis=1, keepdims=True))
    shared_gate_value = jnp.dot(normed, shared_gate_weight, preferred_element_type=jnp.float32)
    shared_up_value = jnp.dot(normed, shared_up_weight, preferred_element_type=jnp.float32)
    shared_hidden = (jax.nn.silu(shared_gate_value) * shared_up_value).astype(jnp.bfloat16)
    shared_total = jnp.dot(shared_hidden, shared_down_weight, preferred_element_type=jnp.float32)
    channel_mixed = (lax.optimization_barrier(jnp.sum(weights[:, :, None] * picked, axis=1)) + shared_total).astype(jnp.bfloat16)
    return (token_mixed, channel_mixed)
```

```python
from collections import namedtuple
from typing import NamedTuple

import jax
import jax.numpy as jnp
from jax import lax
from jax.experimental import pallas as pl
from jax.experimental.pallas import tpu as pltpu
from jax.sharding import Mesh
from jax.sharding import PartitionSpec as P

MESH = pl.DeviceIdType.MESH
F32 = jnp.float32
BF16 = jnp.bfloat16

EPS = 1e-06
TEMPER = 16.0
ROUTED_SCALE = 2.5
BLOCK = 64
RING = 4
EXPERTS = 32
MAIN = 16
LEFT = 2
MAIN_ROWS = EXPERTS * MAIN
SLOTS = EXPERTS * (MAIN + LEFT)
CHUNKS = 4
PER_CHUNK = EXPERTS // CHUNKS
CHUNK_MAIN = PER_CHUNK * MAIN
CHUNK = PER_CHUNK * (MAIN + LEFT)
TOP = 80
TOK_A = 256
TOK_B = 96
COLS = 128
HEAD_K = 64
MIX_ROWS = TOK_A + TOK_B // 2


def nn(a, b):
    return lax.dot_general(a, b, (((1,), (0,)), ((), ())), preferred_element_type=F32)


def nt(a, b):
    return lax.dot_general(a, b, (((1,), (1,)), ((), ())), preferred_element_type=F32)


def tn(a, b):
    return lax.dot_general(a, b, (((0,), (0,)), ((), ())), preferred_element_type=F32)


def silu(a):
    return a / (1.0 + jnp.exp(-a))


def sums_of(value, picks):
    high = value.astype(BF16)
    rest = value - high.astype(F32)
    middle = rest.astype(BF16)
    low = (rest - middle.astype(F32)).astype(BF16)
    return nn(high, picks) + nn(middle, picks) + nn(low, picks)


def as_column(row):
    return jnp.broadcast_to(row, (128, row.shape[1])).T


def split_rows(start, stop):
    return pl.ds(start, stop - start)


class Inputs(NamedTuple):
    q: object
    k: object
    v: object
    og: object
    dec: object
    bias: object
    added: object
    hgain: object
    wo: object
    rows: object
    egain: object
    idx: object
    scores: object
    wg: object
    wu: object
    wd: object
    sg: object
    su: object
    sd: object


def layer_kernel(zs, given, token_mixed, channel_mixed, r):
    z, c = lax.axis_index("z"), lax.axis_index("c")
    y, x = lax.axis_index("y"), lax.axis_index("x")
    experts = zs * 2
    me = z * 2 + c
    tp = y * RING + x

    def turn(a, d):
        return lax.rem(a + d + RING, RING)

    partner = (z, 1 - c, y, x)
    x_up, x_down = (z, c, y, turn(x, 1)), (z, c, y, turn(x, -1))
    y_up, y_down = (z, c, turn(y, 1), x), (z, c, turn(y, -1), x)

    def ep_device(e):
        return (e // 2, lax.rem(e, 2), y, x)

    class Load:
        count = 0

        def __init__(self, source, target):
            self.copy = pltpu.make_async_copy(source, target, r.load_sem.at[Load.count])
            Load.count += 1
            self.copy.start()

    rows_loads = [
        Load(given.rows, r.rows), Load(given.egain, r.egain),
        Load(given.idx, r.idx), Load(given.scores, r.scores),
    ]
    mixer_loads = [
        Load(given.dec, r.dec), Load(given.bias, r.bias), Load(given.added, r.added),
        Load(given.k, r.k), Load(given.v, r.v), Load(given.q, r.q),
        Load(given.og, r.og), Load(given.hgain, r.hgain),
    ]
    shared_loads = [Load(given.sg, r.sgu.at[pl.ds(0, 64)]), Load(given.su, r.sgu.at[pl.ds(64, 64)])]
    gate_loads = [Load(given.wg.at[0], r.wg), Load(given.wu.at[0], r.wu)]
    down_loads = [Load(given.wd.at[y], r.wd1.at[y]), Load(given.wd.at[:, x], r.wd2.at[x])]
    last_loads = [
        Load(given.wo, r.wo), Load(given.sd, r.sd.at[:, 0]), Load(given.sd, r.sd.at[:, 1]),
    ]

    def loaded(group):
        for item in group:
            item.copy.wait()

    r.chip_in[...] = jnp.zeros_like(r.chip_in)
    r.chip_log_in[...] = jnp.zeros_like(r.chip_log_in)
    barrier = pltpu.get_barrier_semaphore()

    def greet(d, carry):
        pl.semaphore_signal(
            barrier, inc=1, device_id=ep_device(lax.rem(me + d, experts)), device_id_type=MESH
        )
        return carry

    lax.fori_loop(1, experts, greet, 0)
    for who in (x_up, x_down, y_up, y_down):
        pl.semaphore_signal(barrier, inc=1, device_id=who, device_id_type=MESH)

    loaded(rows_loads)
    features = r.rows[...].astype(F32)
    scale = lax.rsqrt(jnp.mean(features * features, axis=1, keepdims=True) + EPS)
    r.normed[...] = (features * scale * r.egain[...]).astype(BF16)

    expert_row = lax.broadcasted_iota(jnp.int32, (EXPERTS, TOK_B), 0)
    idx = r.idx[...]
    scores = r.scores[...]
    weights = ROUTED_SCALE * scores / jnp.sum(scores, axis=0, keepdims=True)
    named = jnp.zeros((EXPERTS, TOK_B), F32)
    share = jnp.zeros((EXPERTS, TOK_B), F32)
    for k in range(4):
        hit = idx[k : k + 1] == expert_row
        named = jnp.where(hit, 1.0, named)
        share = jnp.where(hit, weights[k : k + 1], share)
    before = (
        lax.broadcasted_iota(jnp.int32, (TOK_B, TOK_B), 0)
        < lax.broadcasted_iota(jnp.int32, (TOK_B, TOK_B), 1)
    )
    rank = nn(named.astype(BF16), jnp.where(before, 1.0, 0.0).astype(BF16))
    rank = jnp.where(named > 0.0, rank, 100.0).astype(BF16)

    def slot_parts(q):
        whole = q < MAIN_ROWS
        owner = jnp.where(whole, q // MAIN, (q - MAIN_ROWS) // LEFT)
        place = jnp.where(whole, lax.rem(q, MAIN), MAIN + lax.rem(q, LEFT))
        return owner, place

    owner, place = slot_parts(lax.broadcasted_iota(jnp.int32, (SLOTS, EXPERTS), 0))
    spread = owner == lax.broadcasted_iota(jnp.int32, (SLOTS, EXPERTS), 1)
    picks = nn(jnp.where(spread, 1.0, 0.0).astype(BF16), rank)
    picks = jnp.where(picks == place[:, :1].astype(F32), 1.0, 0.0).astype(BF16)
    own_columns = r.normed[:, pl.ds(pl.multiple_of(tp * COLS, COLS), COLS)]
    slots = nn(picks, own_columns)
    r.out_main[...] = slots[:MAIN_ROWS].astype(BF16)

    def store_left(ref, value):
        value = value.astype(BF16)
        for e in range(EXPERTS):
            ref[e] = value[LEFT * e : LEFT * e + LEFT]

    store_left(r.out_left, slots[MAIN_ROWS:])

    owner, place = slot_parts(lax.broadcasted_iota(jnp.int32, (EXPERTS, SLOTS), 1))
    spread = owner == lax.broadcasted_iota(jnp.int32, (EXPERTS, SLOTS), 0)
    spread = jnp.where(spread, 1.0, 0.0).astype(BF16)
    here = tn(rank, spread) == place[:1].astype(F32)
    share_high = share.astype(BF16)
    share_low = (share - share_high.astype(F32)).astype(BF16)
    r.mix_high[...] = jnp.where(here, tn(share_high, spread), 0.0).astype(BF16)
    r.mix_low[...] = jnp.where(here, tn(share_low, spread), 0.0).astype(BF16)

    loaded(mixer_loads)
    logits = r.dec[...].astype(F32) + as_column(r.bias[...])[:, :1]
    log_gate = jnp.minimum(logits, 0.0) - jnp.log1p(jnp.exp(-jnp.abs(logits)))
    decay = log_gate / TEMPER + r.added[...]
    row = lax.broadcasted_iota(jnp.int32, (TOK_A, TOK_A), 0)
    col = lax.broadcasted_iota(jnp.int32, (TOK_A, TOK_A), 1)
    tri = jnp.where((row // BLOCK == col // BLOCK) & (row <= col), 1.0, 0.0).astype(BF16)
    running = sums_of(decay, tri)
    queries = r.q[...].astype(F32) * jnp.exp(running)
    keys = r.k[...].astype(F32)
    raised = (keys * jnp.exp(-running)).astype(BF16)
    lower = lax.broadcasted_iota(jnp.int32, (BLOCK, BLOCK), 1) <= lax.broadcasted_iota(
        jnp.int32, (BLOCK, BLOCK), 0
    )
    state = jnp.zeros((HEAD_K, COLS), F32)
    lead = jnp.zeros((HEAD_K, 1), F32)
    for b in range(TOK_A // BLOCK):
        at = slice(b * BLOCK, (b + 1) * BLOCK)
        total = running[:, (b + 1) * BLOCK - 1 : (b + 1) * BLOCK]
        q_b = queries[:, at].astype(BF16)
        v_b = r.v[at, :]
        marks = jnp.where(lower, tn(q_b, raised[:, at]), 0.0).astype(BF16)
        out_b = nn(marks, v_b)
        if b:
            out_b = out_b + tn(q_b, state.astype(BF16))
        r.head_local[at, :] = out_b
        r.q_lead[b] = (queries[:, at] * jnp.exp(lead)).astype(BF16)
        update = nn((keys[:, at] * jnp.exp(total - running[:, at])).astype(BF16), v_b)
        state = state * jnp.exp(total) + update
        lead = lead + total
    lead = jnp.broadcast_to(lead, (HEAD_K, 128)).T[:1]
    lead = jnp.concatenate([lead, jnp.zeros((1, 128 - HEAD_K), F32)], axis=1)
    r.own_state[...] = state.astype(BF16)
    r.own_log[...] = lead
    loaded(shared_loads)
    shared = nt(r.normed[...], r.sgu[...])
    shared = silu(shared[:, :64]) * shared[:, 64:]
    shared = jnp.concatenate([shared[: TOK_B // 2], shared[TOK_B // 2 :]], axis=1).astype(BF16)
    r.mixed[y, x, pl.ds(TOK_A, TOK_B // 2), :] = shared

    copies = []

    def send(source, target, device):
        n = len(copies)
        copy = pltpu.make_async_remote_copy(
            src_ref=source,
            dst_ref=target,
            send_sem=r.send_sem.at[n],
            recv_sem=r.recv_sem.at[n],
            device_id=device,
            device_id_type=MESH,
        )
        copies.append(copy)
        copy.start()
        return copy

    def main_rows(e):
        return pl.ds(pl.multiple_of(e * MAIN, MAIN), MAIN)

    def distance(k):
        return (k + 1) // 2 * (2 * lax.rem(k, 2) - 1)

    near = zs // 2
    section = r.section

    def pair_of_copies(main_from, main_to, left_from, left_to, sems, device):
        for n, source, target in ((0, main_from, main_to), (1, left_from, left_to)):
            send_sem, recv_sem = sems(n)
            if device is None:
                pltpu.make_async_copy(source, target, recv_sem).start()
            else:
                pltpu.make_async_remote_copy(
                    src_ref=source,
                    dst_ref=target,
                    send_sem=send_sem,
                    recv_sem=recv_sem,
                    device_id=device,
                    device_id_type=MESH,
                ).start()

    def give(e, k, device):
        chunk = 2 * (k // near) + c
        place = lax.rem(k, near)
        pair_of_copies(
            r.out_main.at[main_rows(e)],
            section.at[chunk, y, x, main_rows(place)],
            r.out_left.at[e],
            r.left_in.at[chunk, place],
            lambda n: (r.ep_send.at[0, n], r.ep_recv.at[n, chunk]),
            device,
        )

    def dispatch(i, carry):
        k = jnp.where(i < near, i, zs + near - 1 - i)
        to = lax.rem(z - distance(k) + zs, zs)
        for core in range(2):
            give(to * 2 + core, k, (to, core, y, x))
        return carry

    def give_back(chunk):
        first, core = near * (chunk // 2), chunk % 2

        def one(k, device):
            place = k - first
            to = lax.rem(z + distance(k) + zs, zs)
            pair_of_copies(
                r.back_main.at[chunk, main_rows(place)],
                r.returned.at[main_rows(me)],
                r.back_left.at[chunk, place],
                r.left_back.at[me],
                lambda n: (r.ep_send.at[1, n], r.back_recv.at[n]),
                device,
            )

        if first == 0:

            @pl.when(c == core)
            def _():
                one(jnp.int32(0), None)

            @pl.when(c != core)
            def _():
                one(jnp.int32(0), partner)

        start = 1 if first == 0 else 0

        def step_back(i, carry):
            k = first + near - 1 - i
            one(k, (lax.rem(z + distance(k) + zs, zs), core, y, x))
            return carry

        lax.fori_loop(0, near - start, step_back, 0)

    def arrived(main_ref, left_ref, main_sem, left_sem):
        pltpu.make_async_copy(main_ref, main_ref, main_sem).wait()
        pltpu.make_async_copy(left_ref, left_ref, left_sem).wait()

    def all_sent(sem):
        rest = r.out_main.at[pl.ds(0, (experts - 1) * MAIN)]
        pltpu.make_async_copy(rest, rest, r.ep_send.at[sem, 0]).wait()
        rest = r.out_left.at[pl.ds(0, experts - 1)]
        pltpu.make_async_copy(rest, rest, r.ep_send.at[sem, 1]).wait()

    pl.semaphore_wait(barrier, experts - 1 + 4)
    give(me, jnp.int32(0), None)
    give(z * 2 + 1 - c, jnp.int32(0), partner)
    lax.fori_loop(1, zs, dispatch, 0)
    to_state = send(r.own_state, r.mate_state, partner)
    to_log = send(r.own_log, r.mate_log, partner)

    wd_near = []
    for d, by_y, by_x in ((1, y_up, x_up), (-1, y_down, x_down)):
        wd_near.append(send(given.wd.at[turn(y, d)], r.wd1.at[y], by_y))
        wd_near.append(send(given.wd.at[:, turn(x, d)], r.wd2.at[x], by_x))
    lower_half, upper_half = pl.ds(0, RING // 2), pl.ds(RING // 2, RING // 2)

    def wd_walk():
        y_two, x_two = turn(y, 2), turn(x, 2)
        steps = [
            send(given.wd.at[y_two, lower_half], r.wd1_pass.at[0], y_up),
            send(given.wd.at[lower_half, x_two], r.wd2_pass.at[0], x_up),
            send(given.wd.at[y_two, upper_half], r.wd1_pass.at[1], y_down),
            send(given.wd.at[upper_half, x_two], r.wd2_pass.at[1], x_down),
        ]
        yield
        for copy in steps:
            copy.wait_recv()
        steps = [
            send(r.wd1_pass.at[0], r.wd1.at[turn(y, -1), lower_half], y_up),
            send(r.wd2_pass.at[0], r.wd2.at[turn(x, -1), lower_half], x_up),
            send(r.wd1_pass.at[1], r.wd1.at[turn(y, 1), upper_half], y_down),
            send(r.wd2_pass.at[1], r.wd2.at[turn(x, 1), upper_half], x_down),
        ]
        yield
        for copy in steps + wd_near:
            copy.wait_recv()

    to_state.wait_recv()
    to_log.wait_recv()
    mate = r.mate_state[...].astype(F32)
    mate_log = r.mate_log[...]
    first = jnp.where(c == 0, state, mate)
    second = jnp.where(c == 0, mate, state)
    second_log = jnp.where(c == 0, mate_log, lead)
    chip = as_column(jnp.exp(second_log))[:HEAD_K] * first + second
    low, high = chip[: HEAD_K // 2], chip[HEAD_K // 2 :]
    r.chip_state[...] = jnp.where(c == 0, low, high).astype(BF16)
    r.chip_log[...] = lead + mate_log

    def chip_copies(to):
        device = (to, c, y, x)
        return [
            pltpu.make_async_remote_copy(
                src_ref=source,
                dst_ref=target.at[z],
                send_sem=r.z_send.at[n, to],
                recv_sem=r.z_recv.at[n, z],
                device_id=device,
                device_id_type=MESH,
            )
            for n, source, target in (
                (0, r.chip_state, r.chip_in),
                (1, r.chip_log, r.chip_log_in),
            )
        ]

    def pass_on(to, carry):
        @pl.when(to > z)
        def _():
            for copy in chip_copies(to):
                copy.start()

        return carry

    lax.fori_loop(0, zs, pass_on, 0)

    def gather_part(buf, axis, start, middle, stop):
        whole, top, bottom = split_rows(start, stop), split_rows(start, middle), split_rows(middle, stop)
        if axis == "x":
            block = lambda d, rows: buf.at[y, turn(x, d), rows]
            slab = lambda d, rows: buf.at[turn(y, d), :, rows]
            up, down, then_up, then_down = x_up, x_down, y_up, y_down
        else:
            block = lambda d, rows: buf.at[turn(y, d), x, rows]
            slab = lambda d, rows: buf.at[:, turn(x, d), rows]
            up, down, then_up, then_down = y_up, y_down, x_up, x_down
        for piece, ahead, back in ((block, up, down), (slab, then_up, then_down)):
            a = send(piece(0, whole), piece(0, whole), ahead)
            b = send(piece(0, whole), piece(0, whole), back)
            yield
            a.wait_recv()
            a = send(piece(-1, top), piece(-1, top), ahead)
            b.wait_recv()
            b = send(piece(1, bottom), piece(1, bottom), back)
            yield
            a.wait_recv()
            b.wait_recv()

    def step(*walks):
        for walk in walks:
            next(walk, None)

    def mixer_walk():
        def take(to, carry):
            @pl.when(to < z)
            def _():
                for n, target in ((0, r.chip_in.at[to]), (1, r.chip_log_in.at[to])):
                    pltpu.make_async_copy(target, target, r.z_recv.at[n, to]).wait()

            return carry

        lax.fori_loop(0, zs, take, 0)
        after = jnp.zeros((1, 128), F32)
        factors = []
        for j in range(zs - 1, -1, -1):
            factors.append(jnp.where(j < z, jnp.exp(after), 0.0))
            after = after + jnp.where(j < z, r.chip_log_in[j], 0.0)
        factors = jnp.concatenate(factors[::-1] + [jnp.zeros((128 - zs, 128), F32)], axis=0).T
        factors = jnp.where(c == 0, factors[: HEAD_K // 2], factors[HEAD_K // 2 : HEAD_K])
        incoming = jnp.zeros((HEAD_K // 2, COLS), F32)
        for j in range(zs):
            incoming = incoming + factors[:, j : j + 1] * r.chip_in[j].astype(F32)
        r.incoming[c] = incoming.astype(BF16)
        to_incoming = send(r.incoming.at[c], r.incoming.at[c], partner)
        yield

        to_incoming.wait_recv()
        incoming = jnp.concatenate([r.incoming[0], r.incoming[1]], axis=0).astype(F32)
        incoming = jnp.where(
            c == 0, incoming, as_column(jnp.exp(mate_log))[:HEAD_K] * incoming + mate
        ).astype(BF16)
        heads = [tn(r.q_lead[b], incoming) for b in range(TOK_A // BLOCK)]
        heads = r.head_local[...] + jnp.concatenate(heads, axis=0)
        heads = heads * lax.rsqrt(jnp.mean(heads * heads, axis=1, keepdims=True) + EPS)
        heads = heads * r.hgain[...] * silu(r.og[...].astype(F32))
        r.mixed[y, x, pl.ds(0, TOK_A), :] = heads.astype(BF16)

    def flow(g):
        if g % 2 == 0:
            weight, mine, other = r.wd1, x, y
            ahead_dev, back_dev, then_ahead, then_back = x_up, x_down, y_up, y_down
        else:
            weight, mine, other = r.wd2, y, x
            ahead_dev, back_dev, then_ahead, then_back = y_up, y_down, x_up, x_down
        whole, top, bottom = pl.ds(0, CHUNK), pl.ds(0, TOP), pl.ds(TOP, CHUNK - TOP)
        rows = section.at[g]
        arrived(
            rows.at[y, x, pl.ds(0, CHUNK_MAIN)], r.left_in.at[g], r.ep_recv.at[0, g], r.ep_recv.at[1, g]
        )
        section[g, y, x, pl.ds(CHUNK_MAIN, CHUNK - CHUNK_MAIN), :] = jnp.concatenate(
            [r.left_in[g, e] for e in range(PER_CHUNK)], axis=0
        )
        yield from gather_part(rows, "xy"[g % 2], 0, TOP, CHUNK)
        lhs = jnp.concatenate(
            [section[g, a, b] for a in range(RING) for b in range(RING)], axis=1
        )
        hidden = r.hidden.at[g]
        hidden[mine] = (silu(nn(lhs, r.wg[...])) * nn(lhs, r.wu[...])).astype(BF16)
        piece = lambda d, part: hidden.at[turn(mine, d), part]
        a = send(piece(0, whole), piece(0, whole), ahead_dev)
        b = send(piece(0, whole), piece(0, whole), back_dev)
        yield
        a.wait_recv()
        a = send(piece(-1, top), piece(-1, top), ahead_dev)
        b.wait_recv()
        b = send(piece(1, bottom), piece(1, bottom), back_dev)
        yield
        a.wait_recv()
        b.wait_recv()

        def product(d):
            lhs = jnp.concatenate([hidden[i] for i in range(RING)], axis=1)
            return nn(lhs, weight[turn(other, d)].reshape(RING * 256, COLS))

        far, close = r.far.at[g], r.close.at[g]
        far[...] = product(2).astype(BF16)
        a = send(far.at[top], close.at[top], then_ahead)
        b = send(far.at[bottom], close.at[bottom], then_back)
        part = r.part.at[g]
        part[0] = product(1)
        part[1] = product(-1)
        part[2] = product(0)
        yield
        a.wait_recv()
        part[0, top] = part[0, top] + close[top].astype(F32)
        r.ahead[g] = part[0].astype(BF16)
        a = send(r.ahead.at[g], r.from_back.at[g], then_ahead)
        b.wait_recv()
        part[1, bottom] = part[1, bottom] + close[bottom].astype(F32)
        r.back[g] = part[1].astype(BF16)
        b = send(r.back.at[g], r.from_ahead.at[g], then_back)
        yield
        a.wait_recv()
        b.wait_recv()
        result = part[2] + r.from_back[g].astype(F32) + r.from_ahead[g].astype(F32)
        r.back_main[g] = result[:CHUNK_MAIN].astype(BF16)
        left = result[CHUNK_MAIN:].astype(BF16)
        for e in range(PER_CHUNK):
            r.back_left[g, e] = left[LEFT * e : LEFT * e + LEFT]
        give_back(g)

    def plane_walk():
        walk_a = gather_part(r.mixed, "x", 0, 80, 160)
        walk_b = gather_part(r.mixed, "y", 160, 224, MIX_ROWS)
        for _ in range(4):
            step(walk_a, walk_b)
            yield
        step(walk_a, walk_b)

    f0, f1, f2, f3 = [flow(g) for g in range(CHUNKS)]
    weights_in, mixing, mixed_out = wd_walk(), mixer_walk(), plane_walk()
    loaded(gate_loads)
    step(f0, f1)
    step(weights_in)
    step(f0, f1)
    step(f0, f1)
    step(f2, f3)
    step(weights_in)
    step(mixing)
    step(f0, f1)
    step(f2, f3)
    step(mixing)
    step(f0, f1)
    step(f2, f3)
    step(mixing)
    step(f0, f1)
    step(f2, f3)
    loaded(down_loads)
    step(weights_in)
    step(f0, f1)
    step(f2, f3)
    step(f0, f1)
    step(mixed_out)
    step(f2, f3)
    step(f0, f1)
    step(mixed_out)
    step(f2, f3)
    step(mixed_out)
    step(f2, f3)
    step(mixed_out)
    step(f2, f3)
    step(mixed_out)

    loaded(last_loads)
    mixed = r.mixed
    lhs = jnp.concatenate(
        [mixed[a, b, pl.ds(0, TOK_A), :] for a in range(RING) for b in range(RING)], axis=1
    )
    token_mixed[...] = nn(lhs, r.wo[...]).astype(BF16)
    lhs = jnp.concatenate(
        [mixed[a, b, pl.ds(TOK_A, TOK_B // 2), :] for a in range(RING) for b in range(RING)], axis=1
    )
    lane = lax.rem(lax.broadcasted_iota(jnp.int32, lhs.shape, 1), 128)
    zero = jnp.zeros_like(lhs)
    lhs = jnp.concatenate(
        [jnp.where(lane < 64, lhs, zero), jnp.where(lane < 64, zero, lhs)], axis=0
    )
    shared = nn(lhs, r.sd[...].reshape(2 * RING * RING * 64, COLS))

    returned = r.returned
    arrived(
        returned.at[pl.ds(0, MAIN_ROWS)], r.left_back, r.back_recv.at[0], r.back_recv.at[1]
    )
    returned[pl.ds(MAIN_ROWS, SLOTS - MAIN_ROWS), :] = jnp.concatenate(
        [r.left_back[e] for e in range(EXPERTS)], axis=0
    )
    total = shared + nn(r.mix_high[...], returned[...]) + nn(r.mix_low[...], returned[...])
    channel_mixed[...] = total.astype(BF16)

    for copy in copies:
        copy.wait_send()
    all_sent(0)
    all_sent(1)

    def passed(to, carry):
        @pl.when(to > z)
        def _():
            for copy in chip_copies(to):
                copy.wait_send()

        return carry

    lax.fori_loop(0, zs, passed, 0)


def solution(mesh):
    zs = mesh.shape["ep"] // 2
    torus = Mesh(mesh.devices.reshape(zs, 2, RING, RING), ("z", "c", "y", "x"))
    ep, tp = ("z", "c"), ("y", "x")

    def local(*args):
        given = Inputs(*args)
        given = given._replace(
            q=given.q.T,
            k=given.k.T,
            dec=given.dec.T,
            idx=given.idx.T,
            scores=given.scores.T,
            sg=given.sg.T,
            su=given.su.T,
            bias=given.bias.reshape(1, -1),
            hgain=given.hgain.reshape(1, -1),
            egain=given.egain.reshape(1, -1),
            wd=given.wd.reshape(RING, RING, 256, COLS),
            sd=given.sd.reshape(RING * RING, 64, COLS),
        )
        held = lambda shape, kind=BF16: pltpu.VMEM(shape, kind)
        like = lambda array: pltpu.VMEM(array.shape, array.dtype)
        dma = lambda *shape: pltpu.SemaphoreType.DMA(shape)
        scratch = dict(
            q=like(given.q),
            k=like(given.k),
            v=like(given.v),
            og=like(given.og),
            dec=like(given.dec),
            bias=like(given.bias),
            added=like(given.added),
            hgain=like(given.hgain),
            wo=like(given.wo),
            rows=like(given.rows),
            egain=like(given.egain),
            idx=like(given.idx),
            scores=like(given.scores),
            sgu=held((128, 2048)),
            wg=held((2048, 256)),
            wu=held((2048, 256)),
            wd1=held((RING, RING, 256, COLS)),
            wd2=held((RING, RING, 256, COLS)),
            sd=held((RING * RING, 2, 64, COLS)),
            normed=held((TOK_B, 2048)),
            out_main=held((MAIN_ROWS, COLS)),
            out_left=held((EXPERTS, LEFT, COLS)),
            left_in=held((CHUNKS, PER_CHUNK, LEFT, COLS)),
            section=held((CHUNKS, RING, RING, CHUNK, COLS)),
            mix_high=held((TOK_B, SLOTS)),
            mix_low=held((TOK_B, SLOTS)),
            head_local=held((TOK_A, COLS), F32),
            q_lead=held((TOK_A // BLOCK, HEAD_K, BLOCK)),
            own_state=held((HEAD_K, COLS)),
            mate_state=held((HEAD_K, COLS)),
            own_log=held((1, 128), F32),
            mate_log=held((1, 128), F32),
            chip_state=held((HEAD_K // 2, COLS)),
            chip_log=held((1, 128), F32),
            chip_in=held((zs, HEAD_K // 2, COLS)),
            chip_log_in=held((zs, 1, 128), F32),
            incoming=held((2, HEAD_K // 2, COLS)),
            mixed=held((RING, RING, MIX_ROWS, COLS)),
            hidden=held((CHUNKS, RING, CHUNK, 256)),
            far=held((CHUNKS, CHUNK, COLS)),
            close=held((CHUNKS, CHUNK, COLS)),
            ahead=held((CHUNKS, CHUNK, COLS)),
            back=held((CHUNKS, CHUNK, COLS)),
            from_ahead=held((CHUNKS, CHUNK, COLS)),
            from_back=held((CHUNKS, CHUNK, COLS)),
            part=held((CHUNKS, 3, CHUNK, COLS), F32),
            back_main=held((CHUNKS, CHUNK_MAIN, COLS)),
            back_left=held((CHUNKS, PER_CHUNK, LEFT, COLS)),
            wd1_pass=held((2, RING // 2, 256, COLS)),
            wd2_pass=held((2, RING // 2, 256, COLS)),
            returned=held((SLOTS, COLS)),
            left_back=held((EXPERTS, LEFT, COLS)),
            load_sem=dma(24),
            send_sem=dma(96),
            recv_sem=dma(96),
            ep_send=dma(2, 2),
            ep_recv=dma(2, CHUNKS),
            back_recv=dma(2),
            z_send=dma(2, zs),
            z_recv=dma(2, zs),
        )
        Scratch = namedtuple("Scratch", tuple(scratch))

        def kernel(*refs):
            n = len(given)
            layer_kernel(zs, Inputs(*refs[:n]), refs[n], refs[n + 1], Scratch(*refs[n + 2 :]))

        return pl.pallas_call(
            kernel,
            out_shape=(
                jax.ShapeDtypeStruct((TOK_A, COLS), BF16),
                jax.ShapeDtypeStruct((TOK_B, COLS), BF16),
            ),
            in_specs=[pl.BlockSpec(memory_space=pltpu.HBM)] * len(given),
            out_specs=(pl.BlockSpec(memory_space=pltpu.VMEM),) * 2,
            scratch_shapes=list(scratch.values()),
            compiler_params=pltpu.CompilerParams(
                collective_id=0, has_side_effects=True, vmem_limit_bytes=67043328
            ),
            name="layer",
        )(*given)

    return jax.shard_map(
        local,
        mesh=torus,
        in_specs=(
            P(ep, tp), P(ep, tp), P(ep, tp), P(ep, tp), P(ep, tp), P(tp), P(tp, ep), P(tp),
            P(None, tp), P(ep, None), P(), P(ep, None), P(ep, None), P(ep, None, tp),
            P(ep, None, tp), P(ep, None, tp), P(None, tp), P(None, tp), P(None, tp),
        ),
        out_specs=(P(ep, tp), P(ep, tp)),
        check_vma=False,
    )
```

```python
import math
from collections import namedtuple
from typing import NamedTuple

import jax
import jax.numpy as jnp
from jax import lax
from jax.experimental import pallas as pl
from jax.experimental.pallas import tpu as pltpu
from jax.sharding import Mesh
from jax.sharding import PartitionSpec as P

MESH = pl.DeviceIdType.MESH
F32 = jnp.float32
BF16 = jnp.bfloat16

SENDS, RECEIVES = 14, 53
DIRECT, MDIRECT = (2, 3), True
EPS = 1e-06
TEMPER = 16.0
ROUTED_SCALE = 2.5
BLOCK = 64
RING = 4
EXPERTS = 32
MAIN = 16
LEFT = 2
MAIN_ROWS = EXPERTS * MAIN
SLOTS = EXPERTS * (MAIN + LEFT)
CHUNKS = 4
PER_CHUNK = EXPERTS // CHUNKS
CHUNK_MAIN = PER_CHUNK * MAIN
CHUNK = PER_CHUNK * (MAIN + LEFT)
TOP = 80
TOK_A = 256
TOK_B = 96
COLS = 128
HEAD_K = 64
MIX_ROWS = TOK_A + TOK_B // 2


def nn(a, b):
    return lax.dot_general(a, b, (((1,), (0,)), ((), ())), preferred_element_type=F32)


def nt(a, b):
    return lax.dot_general(a, b, (((1,), (1,)), ((), ())), preferred_element_type=F32)


def tn(a, b):
    return lax.dot_general(a, b, (((0,), (0,)), ((), ())), preferred_element_type=F32)


def silu(a):
    return a / (1.0 + jnp.exp(-a))


def sums_of(value, picks):
    high = value.astype(BF16)
    rest = value - high.astype(F32)
    middle = rest.astype(BF16)
    low = (rest - middle.astype(F32)).astype(BF16)
    return nn(high, picks) + nn(middle, picks) + nn(low, picks)


def as_column(row):
    return jnp.broadcast_to(row, (128, row.shape[1])).T


def split_rows(start, stop):
    return pl.ds(start, stop - start)


class Inputs(NamedTuple):
    q: object
    k: object
    v: object
    og: object
    dec: object
    bias: object
    added: object
    hgain: object
    wo: object
    rows: object
    egain: object
    idx: object
    scores: object
    wg: object
    wu: object
    wd: object
    sg: object
    su: object
    sd: object


def layer_kernel(zs, given, token_mixed, channel_mixed, r):
    z, c = lax.axis_index("z"), lax.axis_index("c")
    y, x = lax.axis_index("y"), lax.axis_index("x")
    experts = zs * 2
    me = z * 2 + c
    tp = y * RING + x

    def turn(a, d):
        return lax.rem(a + d + RING, RING)

    partner = (z, 1 - c, y, x)
    x_up, x_down = (z, c, y, turn(x, 1)), (z, c, y, turn(x, -1))
    y_up, y_down = (z, c, turn(y, 1), x), (z, c, turn(y, -1), x)

    x_far, y_far = (z, c, y, turn(x, 2)), (z, c, turn(y, 2), x)

    def ep_device(e):
        return (e // 2, lax.rem(e, 2), y, x)

    class Load:
        count = 0

        def __init__(self, source, target):
            self.copy = pltpu.make_async_copy(source, target, r.load_sem.at[Load.count])
            Load.count += 1
            self.copy.start()

    rows_loads = [
        Load(given.rows, r.rows), Load(given.egain, r.egain),
        Load(given.idx, r.idx), Load(given.scores, r.scores),
    ]
    r.chip_in[...] = jnp.zeros_like(r.chip_in)
    r.chip_log_in[...] = jnp.zeros_like(r.chip_log_in)
    barrier = pltpu.get_barrier_semaphore()

    def greet(d, carry):
        pl.semaphore_signal(
            barrier, inc=1, device_id=ep_device(lax.rem(me + d, experts)), device_id_type=MESH
        )
        return carry

    lax.fori_loop(1, experts, greet, 0)
    for who in (x_up, x_down, y_up, y_down, x_far, y_far):
        pl.semaphore_signal(barrier, inc=1, device_id=who, device_id_type=MESH)

    mixer_loads = [
        Load(given.dec, r.dec), Load(given.bias, r.bias), Load(given.added, r.added),
        Load(given.k, r.k), Load(given.v, r.v), Load(given.q, r.q),
        Load(given.og, r.og), Load(given.hgain, r.hgain),
    ]
    shared_loads = [Load(given.sg, r.sgu.at[pl.ds(0, 64)]), Load(given.su, r.sgu.at[pl.ds(64, 64)])]
    gate_loads = [Load(given.wg.at[0], r.wg), Load(given.wu.at[0], r.wu)]
    down_loads = [Load(given.wd.at[y], r.wd1.at[y]), Load(given.wd.at[:, x], r.wd2.at[x])]
    last_loads = [
        Load(given.wo, r.wo), Load(given.sd, r.sd.at[:, 0]), Load(given.sd, r.sd.at[:, 1]),
    ]

    def loaded(group):
        for item in group:
            item.copy.wait()

    loaded(rows_loads)
    features = r.rows[...].astype(F32)
    scale = lax.rsqrt(jnp.mean(features * features, axis=1, keepdims=True) + EPS)
    r.normed[...] = (features * scale * r.egain[...]).astype(BF16)

    expert_row = lax.broadcasted_iota(jnp.int32, (EXPERTS, TOK_B), 0)
    idx = r.idx[...]
    scores = r.scores[...]
    weights = ROUTED_SCALE * scores / jnp.sum(scores, axis=0, keepdims=True)
    named = jnp.zeros((EXPERTS, TOK_B), F32)
    share = jnp.zeros((EXPERTS, TOK_B), F32)
    for k in range(4):
        hit = idx[k : k + 1] == expert_row
        named = jnp.where(hit, 1.0, named)
        share = jnp.where(hit, weights[k : k + 1], share)
    before = (
        lax.broadcasted_iota(jnp.int32, (TOK_B, TOK_B), 0)
        < lax.broadcasted_iota(jnp.int32, (TOK_B, TOK_B), 1)
    )
    rank = nn(named.astype(BF16), jnp.where(before, 1.0, 0.0).astype(BF16))
    rank = jnp.where(named > 0.0, rank, 100.0).astype(BF16)

    def slot_parts(q):
        whole = q < MAIN_ROWS
        owner = jnp.where(whole, q // MAIN, (q - MAIN_ROWS) // LEFT)
        place = jnp.where(whole, lax.rem(q, MAIN), MAIN + lax.rem(q, LEFT))
        return owner, place

    owner, place = slot_parts(lax.broadcasted_iota(jnp.int32, (SLOTS, EXPERTS), 0))
    spread = owner == lax.broadcasted_iota(jnp.int32, (SLOTS, EXPERTS), 1)
    picks = nn(jnp.where(spread, 1.0, 0.0).astype(BF16), rank)
    picks = jnp.where(picks == place[:, :1].astype(F32), 1.0, 0.0).astype(BF16)
    own_columns = r.normed[:, pl.ds(pl.multiple_of(tp * COLS, COLS), COLS)]
    slots = nn(picks, own_columns)
    r.out_main[...] = slots[:MAIN_ROWS].astype(BF16)

    def store_left(ref, value):
        value = value.astype(BF16)
        for e in range(EXPERTS):
            ref[e] = value[LEFT * e : LEFT * e + LEFT]

    store_left(r.out_left, slots[MAIN_ROWS:])

    sent_rows = [0]
    receivers = []

    def receiver():
        receivers.append(len(receivers))
        return receivers[-1]

    def send(source, target, device, recv):
        rows = math.prod(source.shape) * source.dtype.itemsize // (2 * COLS)
        if sent_rows[-1] + rows > r.wo.shape[0]:
            sent_rows.append(0)
        sent_rows[-1] += rows
        pltpu.make_async_remote_copy(
            src_ref=source,
            dst_ref=target,
            send_sem=r.send_sem.at[len(sent_rows) - 1],
            recv_sem=r.recv_sem.at[recv],
            device_id=device,
            device_id_type=MESH,
        ).start()

    def landed(ref, recv):
        pltpu.make_async_copy(ref, ref, r.recv_sem.at[recv]).wait()

    def main_rows(e):
        return pl.ds(pl.multiple_of(e * MAIN, MAIN), MAIN)

    def distance(k):
        return (k + 1) // 2 * (2 * lax.rem(k, 2) - 1)

    near = zs // 2
    section = r.section

    def pair_of_copies(main_from, main_to, left_from, left_to, sems, device):
        for n, source, target in ((0, main_from, main_to), (1, left_from, left_to)):
            send_sem, recv_sem = sems(n)
            if device is None:
                pltpu.make_async_copy(source, target, recv_sem).start()
            else:
                pltpu.make_async_remote_copy(
                    src_ref=source,
                    dst_ref=target,
                    send_sem=send_sem,
                    recv_sem=recv_sem,
                    device_id=device,
                    device_id_type=MESH,
                ).start()

    def give(e, k, device):
        chunk = 2 * (k // near) + c
        place = lax.rem(k, near)
        pair_of_copies(
            r.out_main.at[main_rows(e)],
            section.at[chunk, y, x, main_rows(place)],
            r.out_left.at[e],
            r.left_in.at[chunk, place],
            lambda n: (r.ep_send.at[0, n], r.ep_recv.at[n, chunk]),
            device,
        )

    def dispatch(i, carry):
        k = jnp.where(i < near, i, zs + near - 1 - i)
        to = lax.rem(z - distance(k) + zs, zs)
        for core in range(2):
            give(to * 2 + core, k, (to, core, y, x))
        return carry

    def give_back(chunk):
        first, core = near * (chunk // 2), chunk % 2

        def one(k, device):
            place = k - first
            to = lax.rem(z + distance(k) + zs, zs)
            pair_of_copies(
                r.back_main.at[chunk, main_rows(place)],
                r.returned.at[main_rows(me)],
                r.back_left.at[chunk, place],
                r.left_back.at[me],
                lambda n: (r.ep_send.at[1, n], r.back_recv.at[n]),
                device,
            )

        if first == 0:

            @pl.when(c == core)
            def _():
                one(jnp.int32(0), None)

            @pl.when(c != core)
            def _():
                one(jnp.int32(0), partner)

        start = 1 if first == 0 else 0

        def step_back(i, carry):
            k = first + near - 1 - i
            one(k, (lax.rem(z + distance(k) + zs, zs), core, y, x))
            return carry

        lax.fori_loop(0, near - start, step_back, 0)

    def arrived(main_ref, left_ref, main_sem, left_sem):
        pltpu.make_async_copy(main_ref, main_ref, main_sem).wait()
        pltpu.make_async_copy(left_ref, left_ref, left_sem).wait()

    def all_sent(sem):
        rest = r.out_main.at[pl.ds(0, (experts - 1) * MAIN)]
        pltpu.make_async_copy(rest, rest, r.ep_send.at[sem, 0]).wait()
        rest = r.out_left.at[pl.ds(0, experts - 1)]
        pltpu.make_async_copy(rest, rest, r.ep_send.at[sem, 1]).wait()

    pl.semaphore_wait(barrier, experts - 1 + 6)
    give(me, jnp.int32(0), None)
    give(z * 2 + 1 - c, jnp.int32(0), partner)
    lax.fori_loop(1, zs, dispatch, 0)
    def wd_walk():
        y_two, x_two = turn(y, 2), turn(x, 2)
        pass_in = [(receiver(), receiver()) for _ in range(2)]
        wd1_in, wd2_in = receiver(), receiver()
        for j, (by_y, by_x) in enumerate(pass_in):
            for at, y_side, x_side in ((j, y_up, x_up), (j + 2, y_down, x_down)):
                send(given.wd.at[y_two, at], r.wd1_pass.at[at], y_side, by_y)
                send(given.wd.at[at, x_two], r.wd2_pass.at[at], x_side, by_x)
            yield
        for j in range(RING):
            for d, y_side, x_side in ((1, y_up, x_up), (-1, y_down, x_down)):
                send(given.wd.at[turn(y, d), j], r.wd1.at[y, j], y_side, wd1_in)
                send(given.wd.at[j, turn(x, d)], r.wd2.at[x, j], x_side, wd2_in)
            yield
        for j, (by_y, by_x) in enumerate(pass_in):
            landed(r.wd1_pass.at[pl.ds(0, 2)], by_y)
            landed(r.wd2_pass.at[pl.ds(0, 2)], by_x)
            for at, d, y_side, x_side in ((j, -1, y_up, x_up), (j + 2, 1, y_down, x_down)):
                send(r.wd1_pass.at[at], r.wd1.at[turn(y, d), at], y_side, wd1_in)
                send(r.wd2_pass.at[at], r.wd2.at[turn(x, d), at], x_side, wd2_in)
            yield
        landed(r.wd1.at[pl.ds(0, 3)], wd1_in)
        landed(r.wd2.at[pl.ds(0, 3)], wd2_in)

    def step(*walks):
        for walk in walks:
            next(walk, None)

    weights_in = wd_walk()
    step(weights_in)
    step(weights_in)
    step(weights_in)
    step(weights_in)
    step(weights_in)

    loaded(mixer_loads)
    logits = r.dec[...].astype(F32) + as_column(r.bias[...])[:, :1]
    log_gate = jnp.minimum(logits, 0.0) - jnp.log1p(jnp.exp(-jnp.abs(logits)))
    decay = log_gate / TEMPER + r.added[...]
    row = lax.broadcasted_iota(jnp.int32, (TOK_A, TOK_A), 0)
    col = lax.broadcasted_iota(jnp.int32, (TOK_A, TOK_A), 1)
    tri = jnp.where((row // BLOCK == col // BLOCK) & (row <= col), 1.0, 0.0).astype(BF16)
    running = sums_of(decay, tri)
    queries = r.q[...].astype(F32) * jnp.exp(running)
    keys = r.k[...].astype(F32)
    raised = (keys * jnp.exp(-running)).astype(BF16)
    lower = lax.broadcasted_iota(jnp.int32, (BLOCK, BLOCK), 1) <= lax.broadcasted_iota(
        jnp.int32, (BLOCK, BLOCK), 0
    )
    state = jnp.zeros((HEAD_K, COLS), F32)
    lead = jnp.zeros((HEAD_K, 1), F32)
    for b in range(TOK_A // BLOCK):
        at = slice(b * BLOCK, (b + 1) * BLOCK)
        total = running[:, (b + 1) * BLOCK - 1 : (b + 1) * BLOCK]
        q_b = queries[:, at].astype(BF16)
        v_b = r.v[at, :]
        marks = jnp.where(lower, tn(q_b, raised[:, at]), 0.0).astype(BF16)
        out_b = nn(marks, v_b)
        if b:
            out_b = out_b + tn(q_b, state.astype(BF16))
        r.head_local[at, :] = out_b
        r.q_lead[b] = (queries[:, at] * jnp.exp(lead)).astype(BF16)
        update = nn((keys[:, at] * jnp.exp(total - running[:, at])).astype(BF16), v_b)
        state = state * jnp.exp(total) + update
        lead = lead + total
    lead = jnp.broadcast_to(lead, (HEAD_K, 128)).T[:1]
    lead = jnp.concatenate([lead, jnp.zeros((1, 128 - HEAD_K), F32)], axis=1)
    r.own_state[...] = state.astype(BF16)
    r.own_log[...] = jnp.broadcast_to(lead, (8, 128))
    state_in, log_in, incoming_in = receiver(), receiver(), receiver()
    send(r.own_state, r.mate_state, partner, state_in)
    send(r.own_log, r.mate_log, partner, log_in)

    owner, place = slot_parts(lax.broadcasted_iota(jnp.int32, (EXPERTS, SLOTS), 1))
    spread = owner == lax.broadcasted_iota(jnp.int32, (EXPERTS, SLOTS), 0)
    spread = jnp.where(spread, 1.0, 0.0).astype(BF16)
    here = tn(rank, spread) == place[:1].astype(F32)
    share_high = share.astype(BF16)
    share_low = (share - share_high.astype(F32)).astype(BF16)
    r.mix_high[...] = jnp.where(here, tn(share_high, spread), 0.0).astype(BF16)
    r.mix_low[...] = jnp.where(here, tn(share_low, spread), 0.0).astype(BF16)

    loaded(shared_loads)
    shared = nt(r.normed[...], r.sgu[...])
    shared = silu(shared[:, :64]) * shared[:, 64:]
    shared = jnp.concatenate([shared[: TOK_B // 2], shared[TOK_B // 2 :]], axis=1).astype(BF16)
    r.mixed[y, x, pl.ds(TOK_A, TOK_B // 2), :] = shared

    landed(r.mate_state, state_in)
    landed(r.mate_log, log_in)
    mate = r.mate_state[...].astype(F32)
    mate_log = r.mate_log[:1]
    first = jnp.where(c == 0, state, mate)
    second = jnp.where(c == 0, mate, state)
    second_log = jnp.where(c == 0, mate_log, lead)
    chip = as_column(jnp.exp(second_log))[:HEAD_K] * first + second
    low, high = chip[: HEAD_K // 2], chip[HEAD_K // 2 :]
    r.chip_state[...] = jnp.where(c == 0, low, high).astype(BF16)
    r.chip_log[...] = lead + mate_log

    def chip_copies(to):
        device = (to, c, y, x)
        return [
            pltpu.make_async_remote_copy(
                src_ref=source,
                dst_ref=target.at[z],
                send_sem=r.z_send.at[n, to],
                recv_sem=r.z_recv.at[n, z],
                device_id=device,
                device_id_type=MESH,
            )
            for n, source, target in (
                (0, r.chip_state, r.chip_in),
                (1, r.chip_log, r.chip_log_in),
            )
        ]

    def pass_on(to, carry):
        @pl.when(to > z)
        def _():
            for copy in chip_copies(to):
                copy.start()

        return carry

    lax.fori_loop(0, zs, pass_on, 0)

    def gather_part(buf, axis, start, middle, stop, direct):
        whole, top, bottom = split_rows(start, stop), split_rows(start, middle), split_rows(middle, stop)
        if axis == "x":
            block = lambda d, rows: buf.at[y, turn(x, d), rows]
            slab = lambda d, rows: buf.at[turn(y, d), :, rows]
            up, down, far, then_up, then_down = x_up, x_down, x_far, y_up, y_down
        else:
            block = lambda d, rows: buf.at[turn(y, d), x, rows]
            slab = lambda d, rows: buf.at[:, turn(x, d), rows]
            up, down, far, then_up, then_down = y_up, y_down, y_far, x_up, x_down
        from_down, from_up, from_far = receiver(), receiver(), receiver()
        then_from_down, then_from_up, then_from_far = receiver(), receiver(), receiver()

        def out(piece, device, recv):
            send(piece, piece, device, recv)

        def over(d):
            out(block(d, whole), then_up, then_from_down)
            out(block(d, whole), then_down, then_from_up)

        out(block(0, whole), up, from_down)
        out(block(0, whole), down, from_up)
        if direct:
            out(block(0, whole), far, from_far)
        over(0)
        yield
        landed(block(-1, whole), from_down)
        if not direct:
            out(block(-1, top), up, from_far)
        over(-1)
        landed(block(1, whole), from_up)
        if not direct:
            out(block(1, bottom), down, from_far)
        over(1)
        if not direct:
            yield
        landed(block(2, whole), from_far)
        over(2)
        yield
        landed(slab(-1, whole), then_from_down)
        out(slab(-1, top), then_up, then_from_far)
        landed(slab(1, whole), then_from_up)
        out(slab(1, bottom), then_down, then_from_far)
        yield
        landed(slab(2, whole), then_from_far)

    def mixer_walk():
        def take(to, carry):
            @pl.when(to < z)
            def _():
                for n, target in ((0, r.chip_in.at[to]), (1, r.chip_log_in.at[to])):
                    pltpu.make_async_copy(target, target, r.z_recv.at[n, to]).wait()

            return carry

        lax.fori_loop(0, zs, take, 0)
        after = jnp.zeros((1, 128), F32)
        factors = []
        for j in range(zs - 1, -1, -1):
            factors.append(jnp.where(j < z, jnp.exp(after), 0.0))
            after = after + jnp.where(j < z, r.chip_log_in[j], 0.0)
        factors = jnp.concatenate(factors[::-1] + [jnp.zeros((128 - zs, 128), F32)], axis=0).T
        factors = jnp.where(c == 0, factors[: HEAD_K // 2], factors[HEAD_K // 2 : HEAD_K])
        incoming = jnp.zeros((HEAD_K // 2, COLS), F32)
        for j in range(zs):
            incoming = incoming + factors[:, j : j + 1] * r.chip_in[j].astype(F32)
        r.incoming[c] = incoming.astype(BF16)
        send(r.incoming.at[c], r.incoming.at[c], partner, incoming_in)
        yield

        landed(r.incoming.at[1 - c], incoming_in)
        incoming = jnp.concatenate([r.incoming[0], r.incoming[1]], axis=0).astype(F32)
        incoming = jnp.where(
            c == 0, incoming, as_column(jnp.exp(mate_log))[:HEAD_K] * incoming + mate
        ).astype(BF16)
        heads = [tn(r.q_lead[b], incoming) for b in range(TOK_A // BLOCK)]
        heads = r.head_local[...] + jnp.concatenate(heads, axis=0)
        heads = heads * lax.rsqrt(jnp.mean(heads * heads, axis=1, keepdims=True) + EPS)
        heads = heads * r.hgain[...] * silu(r.og[...].astype(F32))
        r.mixed[y, x, pl.ds(0, TOK_A), :] = heads.astype(BF16)

    def flow(g):
        if g % 2 == 0:
            weight, mine, other = r.wd1, x, y
            ahead_dev, back_dev, then_ahead, then_back = x_up, x_down, y_up, y_down
            far_dev, then_far = x_far, y_far
        else:
            weight, mine, other = r.wd2, y, x
            ahead_dev, back_dev, then_ahead, then_back = y_up, y_down, x_up, x_down
            far_dev, then_far = y_far, x_far
        rows = section.at[g]
        arrived(
            rows.at[y, x, pl.ds(0, CHUNK_MAIN)], r.left_in.at[g], r.ep_recv.at[0, g], r.ep_recv.at[1, g]
        )
        section[g, y, x, pl.ds(CHUNK_MAIN, CHUNK - CHUNK_MAIN), :] = jnp.concatenate(
            [r.left_in[g, e] for e in range(PER_CHUNK)], axis=0
        )
        yield from gather_part(rows, "xy"[g % 2], 0, TOP, CHUNK, g in DIRECT)
        lhs = jnp.concatenate(
            [section[g, a, b] for a in range(RING) for b in range(RING)], axis=1
        )
        hidden = r.hidden.at[g]
        hidden[mine] = (silu(nn(lhs, r.wg[...])) * nn(lhs, r.wu[...])).astype(BF16)
        hidden_in, parts_in = receiver(), receiver()
        for device in (far_dev, ahead_dev, back_dev):
            send(hidden.at[mine], hidden.at[mine], device, hidden_in)
        yield
        landed(hidden.at[pl.ds(0, 3)], hidden_in)

        def product(d):
            lhs = jnp.concatenate([hidden[i] for i in range(RING)], axis=1)
            return nn(lhs, weight[turn(other, d)].reshape(RING * 256, COLS))

        for n, d, device in ((0, 2, then_far), (1, 1, then_ahead), (2, -1, then_back)):
            r.part[g, n] = product(d).astype(BF16)
            send(r.part.at[g, n], r.parts_in.at[g, n], device, parts_in)
        r.own_part[g] = product(0)
        yield
        landed(r.parts_in.at[g], parts_in)
        result = r.own_part[g]
        for n in range(3):
            result = result + r.parts_in[g, n].astype(F32)
        r.back_main[g] = result[:CHUNK_MAIN].astype(BF16)
        left = result[CHUNK_MAIN:].astype(BF16)
        for e in range(PER_CHUNK):
            r.back_left[g, e] = left[LEFT * e : LEFT * e + LEFT]
        give_back(g)

    def plane_walk():
        walk_a = gather_part(r.mixed, "x", 0, 80, 160, MDIRECT)
        walk_b = gather_part(r.mixed, "y", 160, 224, MIX_ROWS, MDIRECT)
        for _ in range(3 if MDIRECT else 4):
            step(walk_a, walk_b)
            yield
        step(walk_a, walk_b)

    f0, f1, f2, f3 = [flow(g) for g in range(CHUNKS)]
    mixing, mixed_out = mixer_walk(), plane_walk()
    loaded(gate_loads + down_loads)
    near_chunks, far_chunks = (f0, f1), (f2, f3)
    A, B, W, X, M = near_chunks, far_chunks, (weights_in,), (mixing,), (mixed_out,)
    for walks in (
        A, W, A, B, W, A, X, B, W, A, X, B, W, A, X, B, M, A, B, M, A, B, M, M,
    ):
        step(*walks)

    loaded(last_loads)
    mixed = r.mixed
    lhs = jnp.concatenate(
        [mixed[a, b, pl.ds(0, TOK_A), :] for a in range(RING) for b in range(RING)], axis=1
    )
    token_mixed[...] = nn(lhs, r.wo[...]).astype(BF16)
    lhs = jnp.concatenate(
        [mixed[a, b, pl.ds(TOK_A, TOK_B // 2), :] for a in range(RING) for b in range(RING)], axis=1
    )
    lane = lax.rem(lax.broadcasted_iota(jnp.int32, lhs.shape, 1), 128)
    zero = jnp.zeros_like(lhs)
    lhs = jnp.concatenate(
        [jnp.where(lane < 64, lhs, zero), jnp.where(lane < 64, zero, lhs)], axis=0
    )
    shared = nn(lhs, r.sd[...].reshape(2 * RING * RING * 64, COLS))

    returned = r.returned
    arrived(
        returned.at[pl.ds(0, MAIN_ROWS)], r.left_back, r.back_recv.at[0], r.back_recv.at[1]
    )
    returned[pl.ds(MAIN_ROWS, SLOTS - MAIN_ROWS), :] = jnp.concatenate(
        [r.left_back[e] for e in range(EXPERTS)], axis=0
    )
    total = shared + nn(r.mix_high[...], returned[...]) + nn(r.mix_low[...], returned[...])
    channel_mixed[...] = total.astype(BF16)

    for n, rows in enumerate(sent_rows):
        rows = r.wo.at[pl.ds(0, rows)]
        pltpu.make_async_copy(rows, rows, r.send_sem.at[n]).wait()
    all_sent(0)
    all_sent(1)

    def passed(to, carry):
        @pl.when(to > z)
        def _():
            for copy in chip_copies(to):
                copy.wait_send()

        return carry

    lax.fori_loop(0, zs, passed, 0)


def solution(mesh):
    zs = mesh.shape["ep"] // 2
    torus = Mesh(mesh.devices.reshape(zs, 2, RING, RING), ("z", "c", "y", "x"))
    ep, tp = ("z", "c"), ("y", "x")

    def local(*args):
        given = Inputs(*args)
        given = given._replace(
            q=given.q.T,
            k=given.k.T,
            dec=given.dec.T,
            idx=given.idx.T,
            scores=given.scores.T,
            sg=given.sg.T,
            su=given.su.T,
            bias=given.bias.reshape(1, -1),
            hgain=given.hgain.reshape(1, -1),
            egain=given.egain.reshape(1, -1),
            wd=given.wd.reshape(RING, RING, 256, COLS),
            sd=given.sd.reshape(RING * RING, 64, COLS),
        )
        held = lambda shape, kind=BF16: pltpu.VMEM(shape, kind)
        like = lambda array: pltpu.VMEM(array.shape, array.dtype)
        dma = lambda *shape: pltpu.SemaphoreType.DMA(shape)
        scratch = dict(
            q=like(given.q),
            k=like(given.k),
            v=like(given.v),
            og=like(given.og),
            dec=like(given.dec),
            bias=like(given.bias),
            added=like(given.added),
            hgain=like(given.hgain),
            wo=like(given.wo),
            rows=like(given.rows),
            egain=like(given.egain),
            idx=like(given.idx),
            scores=like(given.scores),
            sgu=held((128, 2048)),
            wg=held((2048, 256)),
            wu=held((2048, 256)),
            wd1=held((RING, RING, 256, COLS)),
            wd2=held((RING, RING, 256, COLS)),
            sd=held((RING * RING, 2, 64, COLS)),
            normed=held((TOK_B, 2048)),
            out_main=held((MAIN_ROWS, COLS)),
            out_left=held((EXPERTS, LEFT, COLS)),
            left_in=held((CHUNKS, PER_CHUNK, LEFT, COLS)),
            section=held((CHUNKS, RING, RING, CHUNK, COLS)),
            mix_high=held((TOK_B, SLOTS)),
            mix_low=held((TOK_B, SLOTS)),
            head_local=held((TOK_A, COLS), F32),
            q_lead=held((TOK_A // BLOCK, HEAD_K, BLOCK)),
            own_state=held((HEAD_K, COLS)),
            mate_state=held((HEAD_K, COLS)),
            own_log=held((8, 128), F32),
            mate_log=held((8, 128), F32),
            chip_state=held((HEAD_K // 2, COLS)),
            chip_log=held((1, 128), F32),
            chip_in=held((zs, HEAD_K // 2, COLS)),
            chip_log_in=held((zs, 1, 128), F32),
            incoming=held((2, HEAD_K // 2, COLS)),
            mixed=held((RING, RING, MIX_ROWS, COLS)),
            hidden=held((CHUNKS, RING, CHUNK, 256)),
            part=held((CHUNKS, 3, CHUNK, COLS)),
            parts_in=held((CHUNKS, 3, CHUNK, COLS)),
            own_part=held((CHUNKS, CHUNK, COLS), F32),
            back_main=held((CHUNKS, CHUNK_MAIN, COLS)),
            back_left=held((CHUNKS, PER_CHUNK, LEFT, COLS)),
            wd1_pass=held((RING, 256, COLS)),
            wd2_pass=held((RING, 256, COLS)),
            returned=held((SLOTS, COLS)),
            left_back=held((EXPERTS, LEFT, COLS)),
            load_sem=dma(21),
            send_sem=dma(SENDS),
            recv_sem=dma(RECEIVES),
            ep_send=dma(2, 2),
            ep_recv=dma(2, CHUNKS),
            back_recv=dma(2),
            z_send=dma(2, zs),
            z_recv=dma(2, zs),
        )
        Scratch = namedtuple("Scratch", tuple(scratch))

        def kernel(*refs):
            n = len(given)
            layer_kernel(zs, Inputs(*refs[:n]), refs[n], refs[n + 1], Scratch(*refs[n + 2 :]))

        return pl.pallas_call(
            kernel,
            out_shape=(
                jax.ShapeDtypeStruct((TOK_A, COLS), BF16),
                jax.ShapeDtypeStruct((TOK_B, COLS), BF16),
            ),
            in_specs=[pl.BlockSpec(memory_space=pltpu.HBM)] * len(given),
            out_specs=(pl.BlockSpec(memory_space=pltpu.VMEM),) * 2,
            scratch_shapes=list(scratch.values()),
            compiler_params=pltpu.CompilerParams(
                collective_id=0, has_side_effects=True, vmem_limit_bytes=67043328
            ),
            name="layer",
        )(*given)

    return jax.shard_map(
        local,
        mesh=torus,
        in_specs=(
            P(ep, tp), P(ep, tp), P(ep, tp), P(ep, tp), P(ep, tp), P(tp), P(tp, ep), P(tp),
            P(None, tp), P(ep, None), P(), P(ep, None), P(ep, None), P(ep, None, tp),
            P(ep, None, tp), P(ep, None, tp), P(None, tp), P(None, tp), P(None, tp),
        ),
        out_specs=(P(ep, tp), P(ep, tp)),
        check_vma=False,
    )
```
